32 devices in a mesh: rep: 2 (over x), fs: 4 (over z), tp: 4 (over y, core).
Axes of the slice: x: 2, y: 2, z: 4, core: 2. Of those that a mesh axis runs over, the one named last changes fastest.
Arguments:
- tokens: bfloat16 [6144, 2048], P(('rep', 'fs'), 'tp'), parts along dimension 0, may hold values from -6 to 6
- mixer_gain: float32 [2048], replicated, may hold values from 0.1 to 1.9
- rec_weight: bfloat16 [2048, 2048], P('fs', 'tp'), may hold values from -0.125 to 0.125
- gate_weight: bfloat16 [2048, 2048], P('fs', 'tp'), may hold values from -0.125 to 0.125
- conv_taps: bfloat16 [4, 2048], P(None, 'tp'), may hold values from -3 to 3
- recur_map: bfloat16 [8, 256, 256], P('tp'), may hold values from -0.375 to 0.375
- input_map: bfloat16 [8, 256, 256], P('tp'), may hold values from -0.375 to 0.375
- decay_param: float32 [2048], P('tp'), may hold values from 3 to 11
- out_weight: bfloat16 [2048, 2048], P('tp', 'fs'), may hold values from -0.5 to 0.5
- mlp_gain: float32 [2048], replicated, may hold values from 0.1 to 1.9
- up_weight: bfloat16 [2048, 8192], P('fs', 'tp'), may hold values from -0.125 to 0.125
- down_weight: bfloat16 [8192, 2048], P('tp', 'fs'), may hold values from -0.0625 to 0.0625
Outputs:
- layer_out: bfloat16 [6144, 2048], P(('rep', 'fs'), 'tp'), parts along dimension 0
The draws below stay inside these ranges and needn't reach their ends.
There are 2 independent parts, one for each index of `rep`. The reference program is written for one: setup_inputs(seed, part) draws one part's arguments, and reference() takes and returns one part's arrays. A program takes and returns all parts, laid end to end along the dimension named above; an argument that names none is the same for every part. Nothing has to cross between parts.
All inputs are finite; a program needn't handle non-finite values.
Results may differ from the reference program's by a relative error of at most 0.022.
Values may be sent and summed in bfloat16 or wider, within the bound.
A program may use at most 64 MiB of HBM per device.

```python
import math
import jax
import jax.numpy as jnp
from jax import lax

D = 2048
D_RNN = 2048
FF = 8192
N_BLOCKS = 8
CONV_W = 4
TOK_DEV = 768
TOKENS = 3072
BLOCK_W = 256
CH_DEV = 512
FF_DEV = 2048


def draw_decay_param(key, part):
    mask_key, slow_key, quick_key = jax.random.split(jax.random.fold_in(key, 17), 3)
    quick_share = 0.5
    is_quick = jax.random.bernoulli(mask_key, quick_share, (D_RNN,))
    slow_rate = jnp.exp(jax.random.uniform(slow_key, (D_RNN,), jnp.float32, math.log(0.05 / TOK_DEV), math.log(0.4 / TOK_DEV)))
    quick_rate = jnp.exp(jax.random.uniform(quick_key, (D_RNN,), jnp.float32, math.log(0.0025), math.log(0.008)))
    chosen_rate = jnp.where(is_quick, quick_rate, slow_rate)
    return (-jnp.log(jnp.expm1(chosen_rate))).astype(jnp.float32)


def level_of(rng, dims, cuts, low, high):
    loudness, own = 1.0, jax.random.fold_in(rng, 6)
    for dim, shards_of in cuts:
        draws = jnp.exp(jax.random.uniform(jax.random.fold_in(own, dim), (shards_of,), jnp.float32, low / len(cuts), high / len(cuts)))
        loudness = loudness * jnp.repeat(draws, dims[dim] // shards_of).reshape([-1 if axis == dim else 1 for axis in range(len(dims))])
    return loudness


def scatter_about(own_key, shape, spread, most, cuts=(), held_as=jnp.bfloat16):
    drawn = spread * jax.random.normal(own_key, shape, jnp.float32)
    if cuts:
        drawn = drawn * level_of(own_key, shape, cuts, -0.22, 0.18)
    return jnp.clip(drawn, -most, most).astype(held_as)


def setup_inputs(seed: int = 0, part: int = 0) -> dict:
    key_of = jax.random.split(jax.random.key(seed), 13)
    part_keys = jax.random.split(jax.random.fold_in(key_of[12], part), 13)
    tokens = scatter_about(part_keys[0], (TOKENS, D), 1.0, 6.0, ((0, 4), (1, 4)))
    mixer_gain = jnp.clip(1.0 + 0.18 * jax.random.normal(key_of[1], (D,), jnp.float32), 0.1, 1.9)
    rec_weight = scatter_about(key_of[2], (D, D_RNN), D ** -0.5, 0.125, ((0, 4), (1, 4)))
    gate_weight = scatter_about(key_of[3], (D, D_RNN), D ** -0.5, 0.125, ((0, 4), (1, 4)))
    conv_taps = scatter_about(key_of[4], (CONV_W, D_RNN), CONV_W ** -0.5, 3.0, ((1, 4),))
    recur_map = scatter_about(key_of[5], (N_BLOCKS, BLOCK_W, BLOCK_W), BLOCK_W ** -0.5, 0.375, ((0, 4),))
    input_map = scatter_about(key_of[6], (N_BLOCKS, BLOCK_W, BLOCK_W), BLOCK_W ** -0.5, 0.375, ((0, 4),))
    decay_param = draw_decay_param(jax.random.fold_in(key_of[12], 71), part)
    out_weight = scatter_about(key_of[8], (D_RNN, D), (D_RNN // 16) ** -0.5, 0.5, ((0, 4), (1, 4)))
    mlp_gain = jnp.clip(1.0 + 0.18 * jax.random.normal(key_of[9], (D,), jnp.float32), 0.1, 1.9)
    up_weight = scatter_about(key_of[10], (D, FF), D ** -0.5, 0.125, ((0, 4), (1, 4)))
    down_weight = scatter_about(key_of[11], (FF, D), FF ** -0.5, 0.0625, ((0, 4), (1, 4)))
    return {"tokens": tokens, "mixer_gain": mixer_gain, "rec_weight": rec_weight, "gate_weight": gate_weight, "conv_taps": conv_taps, "recur_map": recur_map, "input_map": input_map, "decay_param": decay_param, "out_weight": out_weight, "mlp_gain": mlp_gain, "up_weight": up_weight, "down_weight": down_weight}


NORM_EPSILON = 1e-06
GATE_SCALE = 8.0

def rms_rows(full_rows, gain):
    widened = full_rows.astype(jnp.float32)
    inverse = lax.rsqrt(lax.optimization_barrier(jnp.mean(widened * widened, axis=-1, keepdims=True)) + NORM_EPSILON)
    return (widened * inverse * gain.astype(jnp.float32)).astype(jnp.bfloat16)

def causal_taps(branch, conv_taps):
    widened = branch.astype(jnp.float32)
    tap_values = conv_taps.astype(jnp.float32)
    tap_count = tap_values.shape[0]
    length = widened.shape[-2]
    padded = jnp.pad(widened, [(0, 0)] * (widened.ndim - 2) + [(tap_count - 1, 0), (0, 0)])
    running = jnp.zeros_like(widened)
    for offset in range(tap_count):
        running = running + padded[..., offset:offset + length, :] * tap_values[offset]
    return running.astype(jnp.bfloat16)

def combine(earlier, latter):
    return (earlier[0] * latter[0], latter[0] * earlier[1] + latter[1])

def blocked_sum(hidden, weight, block):
    running = jnp.zeros((hidden.shape[0], weight.shape[1]), jnp.float32)
    for offset in range(0, hidden.shape[1], block):
        partial_value = jnp.dot(hidden[:, offset:offset + block], weight[offset:offset + block], preferred_element_type=jnp.float32)
        rounded = lax.optimization_barrier(partial_value.astype(jnp.bfloat16))
        running = running + rounded.astype(jnp.float32)
    return running

def reference(tokens, mixer_gain, rec_weight, gate_weight, conv_taps, recur_map, input_map, decay_param, out_weight, mlp_gain, up_weight, down_weight):
    normed = rms_rows(tokens, mixer_gain)
    branch = jnp.dot(normed, rec_weight, preferred_element_type=jnp.float32).astype(jnp.bfloat16)
    gate_branch = jnp.dot(normed, gate_weight, preferred_element_type=jnp.float32).astype(jnp.bfloat16)
    seq_count = tokens.shape[0] // TOK_DEV
    conv_out = causal_taps(branch.reshape(seq_count, TOK_DEV, D_RNN), conv_taps)
    blocks = conv_out.astype(jnp.float32).reshape(seq_count, TOK_DEV, N_BLOCKS, BLOCK_W)
    recur_gate = jax.nn.sigmoid(jnp.einsum('slnc,ncd->slnd', blocks, recur_map.astype(jnp.float32)).reshape(seq_count, TOK_DEV, D_RNN))
    input_gate = jax.nn.sigmoid(jnp.einsum('slnc,ncd->slnd', blocks, input_map.astype(jnp.float32)).reshape(seq_count, TOK_DEV, D_RNN))
    log_decay = -GATE_SCALE * recur_gate * jax.nn.softplus(-decay_param.astype(jnp.float32))
    decay_rate = jnp.exp(log_decay)
    drive_term = jnp.sqrt(-jnp.expm1(2.0 * log_decay)) * (input_gate * conv_out.astype(jnp.float32))
    _, states = lax.associative_scan(combine, (decay_rate, drive_term), axis=1)
    gate_act = jax.nn.gelu(gate_branch.astype(jnp.float32)).reshape(seq_count, TOK_DEV, D_RNN)
    mixed_out = (states * gate_act).astype(jnp.bfloat16)
    mixed_out = mixed_out.reshape(seq_count * TOK_DEV, D_RNN)
    mixer_out = blocked_sum(mixed_out, out_weight, CH_DEV)
    middle = (tokens.astype(jnp.float32) + mixer_out).astype(jnp.bfloat16)
    normed_mlp = rms_rows(middle, mlp_gain)
    lifted = jnp.dot(normed_mlp, up_weight, preferred_element_type=jnp.float32)
    squared = jnp.square(jax.nn.relu(lifted)).astype(jnp.bfloat16)
    mlp_out = blocked_sum(squared, down_weight, FF_DEV)
    return (middle.astype(jnp.float32) + mlp_out).astype(jnp.bfloat16)
```

```python
import functools

import jax
import jax.numpy as jnp
from jax import lax
from jax.experimental import pallas as pl
from jax.experimental.pallas import tpu as pltpu
from jax.sharding import PartitionSpec as P

NORM_EPSILON = 1e-06
GATE_SCALE = 8.0


def rms_rows(full_rows, gain):
    widened = full_rows.astype(jnp.float32)
    inverse = lax.rsqrt(jnp.mean(widened * widened, axis=-1, keepdims=True) + NORM_EPSILON)
    return (widened * inverse * gain).astype(jnp.bfloat16)


def recurrence_body(branch_ref, gate_ref, taps_ref, recur_ref, input_ref, rate_ref, out_ref):
    length = branch_ref.shape[0]
    widened = branch_ref[...].astype(jnp.float32)
    taps = taps_ref[...].astype(jnp.float32)
    tap_count = taps.shape[0]
    row = lax.broadcasted_iota(jnp.int32, widened.shape, 0)
    running = widened * taps[tap_count - 1 : tap_count, :]
    for back in range(1, tap_count):
        moved = jnp.where(row >= back, pltpu.roll(widened, back, 0), 0.0)
        running = running + moved * taps[tap_count - 1 - back : tap_count - back, :]
    conv_out = running.astype(jnp.bfloat16)
    recur_gate = jax.nn.sigmoid(jnp.dot(conv_out, recur_ref[0], preferred_element_type=jnp.float32))
    input_gate = jax.nn.sigmoid(jnp.dot(conv_out, input_ref[0], preferred_element_type=jnp.float32))
    log_decay = -recur_gate * rate_ref[...]
    decay = jnp.exp(log_decay)
    shrink = jnp.tanh(-log_decay) * (1.0 + decay * decay)
    state = jnp.sqrt(shrink) * (input_gate * conv_out.astype(jnp.float32))
    step = 1
    while step < length:
        held = row >= step
        state = state + decay * jnp.where(held, pltpu.roll(state, step, 0), 0.0)
        decay = decay * jnp.where(held, pltpu.roll(decay, step, 0), 1.0)
        step *= 2
    gate = jax.nn.gelu(gate_ref[...].astype(jnp.float32))
    out_ref[...] = (state * gate).astype(jnp.bfloat16)


def recurrence(branch, gate_branch, conv_taps, recur_map, input_map, decay_param):
    length, channels = branch.shape
    blocks, block_w = recur_map.shape[:2]
    rate = (GATE_SCALE * jax.nn.softplus(-decay_param)).reshape(1, channels)
    rows = pl.BlockSpec((length, block_w), lambda n: (0, n))
    square = pl.BlockSpec((1, block_w, block_w), lambda n: (n, 0, 0))
    return pl.pallas_call(
        recurrence_body,
        grid=(blocks,),
        in_specs=[
            rows,
            rows,
            pl.BlockSpec((conv_taps.shape[0], block_w), lambda n: (0, n)),
            square,
            square,
            pl.BlockSpec((1, block_w), lambda n: (0, n)),
        ],
        out_specs=rows,
        out_shape=jax.ShapeDtypeStruct((length, channels), jnp.bfloat16),
        cost_estimate=pl.CostEstimate(
            flops=4 * length * channels * block_w, bytes_accessed=40 * length * channels, transcendentals=0
        ),
        compiler_params=pltpu.CompilerParams(vmem_limit_bytes=40 * 1024 * 1024),
    )(branch, gate_branch, conv_taps, recur_map, input_map, rate)


def shift(value, axis, count, by):
    return lax.ppermute(value, axis, [(i, (i + by) % count) for i in range(count)])


def gathered(shard, axis, reps, holders):
    depth, width = shard.shape
    part = depth // reps
    rep, me = lax.axis_index("rep"), lax.axis_index("fs")
    full_shape = (depth * holders, width) if axis == 0 else (depth, width * holders)

    def put(whole, piece, holder, first):
        at = (holder * depth + first, 0) if axis == 0 else (first, holder * width)
        return lax.dynamic_update_slice(whole, piece, at)

    mine = lax.dynamic_slice(shard, (rep * part, 0), (part, width))
    arrived = [(by, shift(mine, "fs", holders, by)) for by in range(1, holders)]
    whole = put(jnp.zeros(full_shape, shard.dtype), shard, me, 0)
    for by, piece in arrived:
        holder = lax.rem(me + holders - by, holders)
        whole = put(whole, piece, holder, rep * part)
        for over in range(1, reps):
            other = shift(piece, "rep", reps, over)
            whole = put(whole, other, holder, lax.rem(rep + reps - over, reps) * part)
    return whole


def shards(
    reps,
    holders,
    tokens,
    mixer_gain,
    rec_weight,
    gate_weight,
    conv_taps,
    recur_map,
    input_map,
    decay_param,
    out_weight,
    mlp_gain,
    up_weight,
    down_weight,
):
    rec_full = gathered(rec_weight, 0, reps, holders)
    gate_full = gathered(gate_weight, 0, reps, holders)
    out_full = gathered(out_weight, 1, reps, holders)
    up_full = gathered(up_weight, 0, reps, holders)
    down_full = gathered(down_weight, 1, reps, holders)
    full_rows = lax.all_gather(tokens, "tp", axis=1, tiled=True)
    normed = rms_rows(full_rows, mixer_gain)
    branch = jnp.dot(normed, rec_full, preferred_element_type=jnp.float32).astype(jnp.bfloat16)
    gate_branch = jnp.dot(normed, gate_full, preferred_element_type=jnp.float32).astype(jnp.bfloat16)
    mixed_out = recurrence(branch, gate_branch, conv_taps, recur_map, input_map, decay_param)
    mixer_terms = jnp.dot(mixed_out, out_full, preferred_element_type=jnp.float32)
    mixer_out = lax.psum_scatter(
        mixer_terms.astype(jnp.bfloat16), "tp", scatter_dimension=1, tiled=True
    ).astype(jnp.float32)
    middle = (tokens.astype(jnp.float32) + mixer_out).astype(jnp.bfloat16)
    middle_rows = lax.all_gather(middle, "tp", axis=1, tiled=True)
    normed_mlp = rms_rows(middle_rows, mlp_gain)
    lifted = jnp.dot(normed_mlp, up_full, preferred_element_type=jnp.float32)
    squared = jnp.square(jax.nn.relu(lifted)).astype(jnp.bfloat16)
    mlp_terms = jnp.dot(squared, down_full, preferred_element_type=jnp.float32)
    mlp_out = lax.psum_scatter(
        mlp_terms.astype(jnp.bfloat16), "tp", scatter_dimension=1, tiled=True
    ).astype(jnp.float32)
    return (middle.astype(jnp.float32) + mlp_out).astype(jnp.bfloat16)


def solution(mesh):
    placed = (
        P(("rep", "fs"), "tp"),
        P(),
        P("fs", "tp"),
        P("fs", "tp"),
        P(None, "tp"),
        P("tp", None, None),
        P("tp", None, None),
        P("tp"),
        P("tp", "fs"),
        P(),
        P("fs", "tp"),
        P("tp", "fs"),
    )
    return jax.shard_map(
        functools.partial(shards, mesh.shape["rep"], mesh.shape["fs"]),
        mesh=mesh,
        in_specs=placed,
        out_specs=P(("rep", "fs"), "tp"),
        check_vma=False,
    )
```
